32 devices in a mesh: sp: 8 (over z, x), tp: 4 (over y, core).
Axes of the slice: x: 2, y: 2, z: 4, core: 2. Of those that a mesh axis runs over, the one named last changes fastest.
Arguments:
- residual: bfloat16 [2048, 2048], P(('sp', 'tp')), may hold values from -6 to 6
- queries: bfloat16 [2048, 1024], P('sp', 'tp'), may hold values from -8 to 8
- key_pairs: bfloat16 [2048, 512], P('sp', 'tp'), may hold values from -8 to 8
- values: bfloat16 [2048, 512], P('sp', 'tp'), may hold values from -6 to 6
- lambdas: float32 [8], P('tp'), may hold values from 0.3 to 0.8
- head_gain: float32 [128], replicated, may hold values from 0.1 to 1.9
- out_weight: bfloat16 [1024, 2048], replicated, may hold values from -0.1875 to 0.1875
- mixer_gain: float32 [2048], replicated, may hold values from 0.1 to 1.9
- before_gain: float32 [2048], replicated, may hold values from 0.1 to 1.9
- after_gain: float32 [2048], replicated, may hold values from 0.1 to 1.9
- gate_weight: bfloat16 [2048, 5632], P('sp', 'tp'), may hold values from -0.125 to 0.125
- up_weight: bfloat16 [2048, 5632], P('sp', 'tp'), may hold values from -0.125 to 0.125
- down_weight: bfloat16 [5632, 2048], P('tp', 'sp'), may hold values from -0.078125 to 0.078125
Outputs:
- updated: bfloat16 [2048, 2048], P(('sp', 'tp'))
The draws below stay inside these ranges and needn't reach their ends.
All inputs are finite; a program needn't handle non-finite values.
Results may differ from the reference program's by a relative error of at most 0.014.
Values may be sent and summed in bfloat16 or wider, within the bound.
A program may use at most 128 MiB of HBM per device.

```python
import math
import jax
import jax.numpy as jnp
from jax import lax

D = 2048
FF = 5632
HEADS = 8
KV_HEADS = 4
HEAD_DIM = 64
TOKENS = 2048
N_TP = 4


def drawn_pair(key):
    query_key, key_key = jax.random.split(key, 2)
    query_draw = jnp.clip(1.3 * jax.random.normal(query_key, (TOKENS, HEADS, 2, HEAD_DIM), jnp.float32), -7.5, 7.5)
    key_draw = jnp.clip(1.3 * jax.random.normal(key_key, (TOKENS, KV_HEADS, 2, HEAD_DIM), jnp.float32), -7.5, 7.5)
    return (query_draw, key_draw)


def draw_queries(key, part):
    query_draw = drawn_pair(jax.random.fold_in(key, 17))[0]
    return query_draw.reshape(TOKENS, HEADS * 2 * HEAD_DIM).astype(jnp.bfloat16)


def draw_key_pairs(key, part):
    key_draw = drawn_pair(jax.random.fold_in(key, 17))[1]
    return key_draw.reshape(TOKENS, KV_HEADS * 2 * HEAD_DIM).astype(jnp.bfloat16)


def level_of(rng, dims, cuts, low, largest):
    loudness, own = 1.0, jax.random.fold_in(rng, 6)
    for axis_at, shards_of in cuts:
        draws = jnp.exp(jax.random.uniform(jax.random.fold_in(own, axis_at), (shards_of,), jnp.float32, low / len(cuts), largest / len(cuts)))
        loudness = loudness * jnp.repeat(draws, dims[axis_at] // shards_of).reshape([-1 if axis == axis_at else 1 for axis in range(len(dims))])
    return loudness


def normal_values(own_key, shape, scale, bound, shards=(), held_as=jnp.bfloat16):
    level = level_of(own_key, shape, shards, -0.22, 0.18) if shards else 1.0
    values = jax.random.normal(own_key, shape, jnp.float32) * scale * level
    return jnp.minimum(jnp.maximum(values, -bound), bound).astype(held_as)


def setup_inputs(seed: int = 0) -> dict:
    arg_keys = jax.random.split(jax.random.key(seed), 14)
    residual = normal_values(arg_keys[0], (TOKENS, D), 1.0, 6.0, ((0, 32),))
    queries = draw_queries(jax.random.fold_in(arg_keys[13], 71), 0)
    key_pairs = draw_key_pairs(jax.random.fold_in(arg_keys[13], 71), 0)
    values = normal_values(arg_keys[3], (TOKENS, KV_HEADS * 2 * HEAD_DIM), 1.0, 6.0, ((0, 8), (1, 4)))
    lambdas = jnp.clip(0.3 + 0.5 * jax.random.uniform(arg_keys[4], (HEADS,), jnp.float32) ** level_of(arg_keys[4], (HEADS,), ((0, 4),), -0.2, 0.2), 0.3, 0.8)
    head_gain = jnp.clip(1.0 + 0.18 * jax.random.normal(arg_keys[5], (2 * HEAD_DIM,), jnp.float32), 0.1, 1.9)
    out_weight = normal_values(arg_keys[6], (HEADS * 2 * HEAD_DIM, D), (HEADS * 2 * HEAD_DIM) ** -0.5, 0.1875)
    mixer_gain = jnp.clip(1.0 + 0.18 * jax.random.normal(arg_keys[7], (D,), jnp.float32), 0.1, 1.9)
    before_gain = jnp.clip(1.0 + 0.18 * jax.random.normal(arg_keys[8], (D,), jnp.float32), 0.1, 1.9)
    after_gain = jnp.clip(1.0 + 0.18 * jax.random.normal(arg_keys[9], (D,), jnp.float32), 0.1, 1.9)
    gate_weight = normal_values(arg_keys[10], (D, FF), D ** -0.5, 0.125, ((0, 8), (1, 4)))
    up_weight = normal_values(arg_keys[11], (D, FF), D ** -0.5, 0.125, ((0, 8), (1, 4)))
    down_weight = normal_values(arg_keys[12], (FF, D), FF ** -0.5, 0.078125, ((0, 4), (1, 8)))
    return {"residual": residual, "queries": queries, "key_pairs": key_pairs, "values": values, "lambdas": lambdas, "head_gain": head_gain, "out_weight": out_weight, "mixer_gain": mixer_gain, "before_gain": before_gain, "after_gain": after_gain, "gate_weight": gate_weight, "up_weight": up_weight, "down_weight": down_weight}


def row_norm(values_in, gain, epsilon):
    mean_square = lax.optimization_barrier(jnp.mean(values_in * values_in, axis=-1, keepdims=True))
    return values_in * lax.rsqrt(mean_square + epsilon) * gain

def reference(residual, queries, key_pairs, values, lambdas, head_gain, out_weight, mixer_gain, before_gain, after_gain, gate_weight, up_weight, down_weight):
    group = HEADS // KV_HEADS
    scale = 1.0 / math.sqrt(HEAD_DIM)
    width = 2 * HEAD_DIM
    query_heads = jnp.transpose(queries.reshape(TOKENS, HEADS, 2, HEAD_DIM), (1, 2, 0, 3))
    key_heads = jnp.transpose(key_pairs.reshape(TOKENS, KV_HEADS, 2, HEAD_DIM), (1, 2, 0, 3))
    value_heads = jnp.transpose(values.reshape(TOKENS, KV_HEADS, width), (1, 0, 2))
    height = math.gcd(TOKENS, 512)
    blocks = TOKENS // height

    def one_block(index):
        head = index // blocks
        first = index % blocks * height
        shared = head // group
        zero = jnp.zeros((), jnp.int32)
        query_block = lax.dynamic_slice(query_heads, (head, zero, first, zero), (1, 2, height, HEAD_DIM))[0]
        key_block = lax.dynamic_index_in_dim(key_heads, shared, 0, keepdims=False)
        value_block = lax.dynamic_index_in_dim(value_heads, shared, 0, keepdims=False)
        second_weight = lax.dynamic_index_in_dim(lambdas, head, 0, keepdims=False)
        results = []
        for which in range(2):
            score = jnp.dot(query_block[which], key_block[which].T, preferred_element_type=jnp.float32) * scale
            top = lax.optimization_barrier(jnp.max(score, axis=1, keepdims=True))
            expo = jnp.exp(score - top)
            total = lax.optimization_barrier(jnp.sum(expo, axis=1, keepdims=True))
            numer = jnp.dot(expo.astype(jnp.bfloat16), value_block, preferred_element_type=jnp.float32)
            results.append(numer / total)
        attended = results[0] - second_weight * results[1]
        return row_norm(attended, head_gain, 1e-05).astype(jnp.bfloat16)
    normed = lax.map(one_block, jnp.arange(HEADS * blocks, dtype=jnp.int32))
    head_out = jnp.transpose(normed.reshape(HEADS, TOKENS, width), (1, 0, 2)).reshape(TOKENS, HEADS * width)
    mixed = jnp.dot(head_out, out_weight, preferred_element_type=jnp.float32).astype(jnp.bfloat16)
    stream = residual.astype(jnp.float32) + row_norm(mixed.astype(jnp.float32), mixer_gain, 1e-06)
    normed_in = row_norm(stream, before_gain, 1e-06).astype(jnp.bfloat16)
    gate = jnp.dot(normed_in, gate_weight, preferred_element_type=jnp.float32)
    up = jnp.dot(normed_in, up_weight, preferred_element_type=jnp.float32)
    hidden = (jax.nn.silu(gate) * up).astype(jnp.bfloat16)
    group_width = FF // N_TP
    channel = jnp.zeros((TOKENS, D), jnp.float32)
    for member in range(N_TP):
        lower = member * group_width
        upper = lower + group_width
        term = jnp.dot(hidden[:, lower:upper], down_weight[lower:upper], preferred_element_type=jnp.float32).astype(jnp.bfloat16)
        channel = channel + lax.optimization_barrier(term).astype(jnp.float32)
    channel = channel.astype(jnp.bfloat16)
    updated = stream + 0.5 * row_norm(channel.astype(jnp.float32), after_gain, 1e-06)
    return updated.astype(jnp.bfloat16)
```

```python
import math

import jax
import jax.numpy as jnp
from jax import lax
from jax.sharding import PartitionSpec as P

HEAD_DIM = 64


def row_norm(values_in, gain, epsilon):
    mean_square = jnp.mean(values_in * values_in, axis=-1, keepdims=True)
    return values_in * lax.rsqrt(mean_square + epsilon) * gain


def on_device(
    residual,
    queries,
    key_pairs,
    values,
    lambdas,
    head_gain,
    out_weight,
    mixer_gain,
    before_gain,
    after_gain,
    gate_weight,
    up_weight,
    down_weight,
):
    tokens_here = queries.shape[0]
    quarter = residual.shape[0]
    width = 2 * HEAD_DIM
    local_heads = queries.shape[1] // width
    scale = 1.0 / math.sqrt(HEAD_DIM)
    height = local_heads * tokens_here
    query_rows = jnp.transpose(
        queries.reshape(tokens_here, local_heads, 2, HEAD_DIM), (2, 1, 0, 3)
    ).reshape(2, height, HEAD_DIM)
    empty = (
        jnp.full((height,), -1e30, jnp.float32),
        jnp.zeros((height,), jnp.float32),
        jnp.zeros((height, width), jnp.float32),
    )
    state = (empty, empty)
    key_piece = lax.all_gather(key_pairs, "sp", axis=0, tiled=True)
    value_piece = lax.all_gather(values, "sp", axis=0, tiled=True)
    length = key_piece.shape[0]
    span = length
    for split_count in range(1, length + 1):
        if length % split_count == 0 and length // split_count <= 2048:
            span = length // split_count
            break
    key_blocks = key_piece.reshape(length // span, span, 2, HEAD_DIM)
    value_blocks = value_piece.reshape(length // span, span, width)

    def advance(carry, blocks_in):
        key_block, value_block = blocks_in
        renewed = []
        for which in range(2):
            running_top, running_total, running_numer = carry[which]
            score = (
                jnp.dot(
                    query_rows[which], key_block[:, which].T, preferred_element_type=jnp.float32
                )
                * scale
            )
            new_top = jnp.maximum(running_top, jnp.max(score, axis=1))
            shrink = jnp.exp(running_top - new_top)
            expo = jnp.exp(score - new_top[:, None])
            new_total = running_total * shrink + jnp.sum(expo, axis=1)
            new_numer = running_numer * shrink[:, None] + jnp.dot(
                expo.astype(jnp.bfloat16), value_block, preferred_element_type=jnp.float32
            )
            renewed.append((new_top, new_total, new_numer))
        return (tuple(renewed), None)

    state, _ = lax.scan(advance, state, (key_blocks, value_blocks))
    first_map, second_map = state
    lambda_rows = jnp.repeat(lambdas, tokens_here)[:, None]
    attended = first_map[2] / first_map[1][:, None] - lambda_rows * (
        second_map[2] / second_map[1][:, None]
    )
    normed = row_norm(attended, head_gain, 1e-05).astype(jnp.bfloat16)
    head_out = jnp.transpose(normed.reshape(local_heads, tokens_here, width), (1, 0, 2)).reshape(
        tokens_here, local_heads * width
    )
    grouped = head_out.reshape(lax.axis_size("tp"), quarter, local_heads * width)
    mixed = jnp.dot(
        lax.all_to_all(grouped, "tp", split_axis=0, concat_axis=2, tiled=True)[0],
        out_weight,
        preferred_element_type=jnp.float32,
    ).astype(jnp.bfloat16)[None][0]
    stream = residual.astype(jnp.float32) + row_norm(mixed.astype(jnp.float32), mixer_gain, 1e-06)
    normed_in = row_norm(stream, before_gain, 1e-06).astype(jnp.bfloat16)
    gathered = lax.all_gather(normed_in, "tp", axis=0, tiled=True)
    empty_hidden = jnp.zeros((gathered.shape[0], gate_weight.shape[1]), jnp.float32)
    pieces = (
        lax.all_gather(gate_weight, "sp", axis=0, tiled=True),
        lax.all_gather(up_weight, "sp", axis=0, tiled=True),
    )
    columns = lax.slice_in_dim(gathered, 0, pieces[0].shape[0], axis=1)
    gate_part = jnp.dot(columns, pieces[0], preferred_element_type=jnp.float32)
    up_part = jnp.dot(columns, pieces[1], preferred_element_type=jnp.float32)
    gate = empty_hidden + gate_part
    up = empty_hidden + up_part
    down_whole = lax.all_gather(down_weight, "sp", axis=1, tiled=True)
    hidden = (jax.nn.silu(gate) * up).astype(jnp.bfloat16)
    picked = lax.slice_in_dim(hidden, 0, lax.axis_size("tp") * quarter, axis=0)
    channel = lax.psum_scatter(
        jnp.dot(picked, down_whole, preferred_element_type=jnp.float32).astype(jnp.bfloat16),
        "tp",
        scatter_dimension=0,
        tiled=True,
    )
    updated = stream + 0.5 * row_norm(channel.astype(jnp.float32), after_gain, 1e-06)
    return updated.astype(jnp.bfloat16)


def swap(block, axis, bits):
    size = lax.axis_size(axis)
    return lax.ppermute(block, axis, [(i, i ^ bits) for i in range(size)])


def placed(blocks, base, axis):
    span = blocks[0].shape[axis]
    shape = list(blocks[0].shape)
    shape[axis] = span * len(blocks)
    whole = jnp.zeros(shape, blocks[0].dtype)
    for j, block in enumerate(blocks):
        whole = lax.dynamic_update_slice_in_dim(whole, block, (base ^ j) * span, axis)
    return whole


def attend(queries, keys, vals, lambdas, head_gain):
    tokens_here = queries.shape[0]
    width = 2 * HEAD_DIM
    local_heads = queries.shape[1] // width
    scale = 1.0 / math.sqrt(HEAD_DIM)
    height = local_heads * tokens_here
    query_rows = jnp.transpose(
        queries.reshape(tokens_here, local_heads, 2, HEAD_DIM), (2, 1, 0, 3)
    ).reshape(2, height, HEAD_DIM)
    parts = []
    for which in range(2):
        key = keys[:, which * HEAD_DIM : (which + 1) * HEAD_DIM]
        score = jnp.dot(query_rows[which], key.T, preferred_element_type=jnp.float32) * scale
        expo = jnp.exp(score - jnp.max(score, axis=1, keepdims=True))
        total = jnp.sum(expo, axis=1, keepdims=True)
        numer = jnp.dot(expo.astype(jnp.bfloat16), vals, preferred_element_type=jnp.float32)
        parts.append(numer / total)
    attended = parts[0] - jnp.repeat(lambdas, tokens_here)[:, None] * parts[1]
    normed = row_norm(attended, head_gain, 1e-05).astype(jnp.bfloat16)
    return normed.reshape(local_heads, tokens_here, width)


def split_units(
    residual,
    queries,
    key_pairs,
    values,
    lambdas,
    head_gain,
    out_weight,
    mixer_gain,
    before_gain,
    after_gain,
    gate_weight,
    up_weight,
    down_weight,
):
    n_sp, n_tp = lax.axis_size("sp"), lax.axis_size("tp")
    depth = n_sp // 2
    place, member = lax.axis_index("sp"), lax.axis_index("tp")
    level, side = place // 2, place % 2
    quarter = residual.shape[0]
    width = 2 * HEAD_DIM
    local_heads = queries.shape[1] // width

    pair = jnp.concatenate([key_pairs, values], axis=1)
    column = [pair] + [swap(pair, "sp", 2 * j) for j in range(1, depth)]
    row = [swap(piece, "sp", 1) for piece in column]
    whole = jnp.concatenate(column + row, axis=0)
    normed = attend(queries, whole[:, :width], whole[:, width:], lambdas, head_gain)

    units = gate_weight.shape[1] // depth

    def scattered(weight, axis):
        mine = []
        for j in range(depth):
            piece = lax.dynamic_slice_in_dim(weight, (level ^ j) * units, units, 1 - axis)
            mine.append(piece if j == 0 else swap(piece, "sp", 2 * j))
        other = [swap(piece, "sp", 1) for piece in mine]
        ordered = []
        for j in range(depth):
            ordered += [mine[j], other[j]]
        return placed(ordered, place, axis)

    gate_mine = scattered(gate_weight, 0)
    up_mine = scattered(up_weight, 0)
    down_mine = scattered(down_weight, 1)

    heads = normed.reshape(local_heads, n_tp, quarter, width)
    sent = []
    for j in range(n_tp):
        block = lax.dynamic_index_in_dim(heads, member ^ j, 1, keepdims=False)
        block = jnp.transpose(block, (1, 0, 2)).reshape(quarter, local_heads * width)
        sent.append(block if j == 0 else swap(block, "tp", j))
    head_out = placed(sent, member, 1)
    mixed = jnp.dot(head_out, out_weight, preferred_element_type=jnp.float32).astype(jnp.bfloat16)
    stream = residual.astype(jnp.float32) + row_norm(mixed.astype(jnp.float32), mixer_gain, 1e-06)
    normed_in = row_norm(stream, before_gain, 1e-06).astype(jnp.bfloat16)

    line = [normed_in] + [swap(normed_in, "sp", 2 * j) for j in range(1, depth)]
    plane = line + [swap(piece, "tp", 2) for piece in line]
    rows = jnp.concatenate(plane, axis=0)
    rows = jnp.concatenate([rows, swap(rows, "tp", 1)], axis=0)

    gate = jnp.dot(rows, gate_mine, preferred_element_type=jnp.float32)
    up = jnp.dot(rows, up_mine, preferred_element_type=jnp.float32)
    hidden = (jax.nn.silu(gate) * up).astype(jnp.bfloat16)

    chunks = 2
    span = down_mine.shape[1] // chunks
    sums = []
    for c in range(chunks):
        part = jnp.dot(
            hidden, down_mine[:, c * span : (c + 1) * span], preferred_element_type=jnp.float32
        )
        half = part.shape[0] // 2
        part = part[:half] + swap(part[half:].astype(jnp.bfloat16), "tp", 1).astype(jnp.float32)
        half = half // 2
        part = part[:half] + swap(part[half:].astype(jnp.bfloat16), "tp", 2).astype(jnp.float32)
        total = part[:quarter]
        for j in range(1, depth):
            block = part[j * quarter : (j + 1) * quarter].astype(jnp.bfloat16)
            total = total + swap(block, "sp", 2 * j).astype(jnp.float32)
        sums.append(total)
    channel = jnp.concatenate(sums, axis=1).astype(jnp.bfloat16)
    updated = stream + 0.5 * row_norm(channel.astype(jnp.float32), after_gain, 1e-06)
    return updated.astype(jnp.bfloat16)


def fits(mesh):
    return mesh.shape["tp"] == 4 and mesh.shape["sp"] == 8


def solution(mesh):
    return jax.shard_map(
        split_units if fits(mesh) else on_device,
        mesh=mesh,
        in_specs=(
            P(("sp", "tp"), None),
            P("sp", "tp"),
            P("sp", "tp"),
            P("sp", "tp"),
            P("tp"),
            P(),
            P(),
            P(),
            P(),
            P(),
            P("sp", "tp"),
            P("sp", "tp"),
            P("tp", "sp"),
        ),
        out_specs=P(("sp", "tp"), None),
        check_vma=False,
    )
```

```python
import math

import jax
import jax.numpy as jnp
from jax import lax
from jax.experimental import pallas as pl
from jax.experimental.pallas import tpu as pltpu
from jax.sharding import PartitionSpec as P

HEAD_DIM = 64


def row_norm(values_in, gain, epsilon):
    mean_square = jnp.mean(values_in * values_in, axis=-1, keepdims=True)
    return values_in * lax.rsqrt(mean_square + epsilon) * gain


def on_device(
    residual,
    queries,
    key_pairs,
    values,
    lambdas,
    head_gain,
    out_weight,
    mixer_gain,
    before_gain,
    after_gain,
    gate_weight,
    up_weight,
    down_weight,
):
    tokens_here = queries.shape[0]
    quarter = residual.shape[0]
    width = 2 * HEAD_DIM
    local_heads = queries.shape[1] // width
    scale = 1.0 / math.sqrt(HEAD_DIM)
    height = local_heads * tokens_here
    query_rows = jnp.transpose(
        queries.reshape(tokens_here, local_heads, 2, HEAD_DIM), (2, 1, 0, 3)
    ).reshape(2, height, HEAD_DIM)
    empty = (
        jnp.full((height,), -1e30, jnp.float32),
        jnp.zeros((height,), jnp.float32),
        jnp.zeros((height, width), jnp.float32),
    )
    state = (empty, empty)
    key_piece = lax.all_gather(key_pairs, "sp", axis=0, tiled=True)
    value_piece = lax.all_gather(values, "sp", axis=0, tiled=True)
    length = key_piece.shape[0]
    span = length
    for split_count in range(1, length + 1):
        if length % split_count == 0 and length // split_count <= 2048:
            span = length // split_count
            break
    key_blocks = key_piece.reshape(length // span, span, 2, HEAD_DIM)
    value_blocks = value_piece.reshape(length // span, span, width)

    def advance(carry, blocks_in):
        key_block, value_block = blocks_in
        renewed = []
        for which in range(2):
            running_top, running_total, running_numer = carry[which]
            score = (
                jnp.dot(
                    query_rows[which], key_block[:, which].T, preferred_element_type=jnp.float32
                )
                * scale
            )
            new_top = jnp.maximum(running_top, jnp.max(score, axis=1))
            shrink = jnp.exp(running_top - new_top)
            expo = jnp.exp(score - new_top[:, None])
            new_total = running_total * shrink + jnp.sum(expo, axis=1)
            new_numer = running_numer * shrink[:, None] + jnp.dot(
                expo.astype(jnp.bfloat16), value_block, preferred_element_type=jnp.float32
            )
            renewed.append((new_top, new_total, new_numer))
        return (tuple(renewed), None)

    state, _ = lax.scan(advance, state, (key_blocks, value_blocks))
    first_map, second_map = state
    lambda_rows = jnp.repeat(lambdas, tokens_here)[:, None]
    attended = first_map[2] / first_map[1][:, None] - lambda_rows * (
        second_map[2] / second_map[1][:, None]
    )
    normed = row_norm(attended, head_gain, 1e-05).astype(jnp.bfloat16)
    head_out = jnp.transpose(normed.reshape(local_heads, tokens_here, width), (1, 0, 2)).reshape(
        tokens_here, local_heads * width
    )
    grouped = head_out.reshape(lax.axis_size("tp"), quarter, local_heads * width)
    mixed = jnp.dot(
        lax.all_to_all(grouped, "tp", split_axis=0, concat_axis=2, tiled=True)[0],
        out_weight,
        preferred_element_type=jnp.float32,
    ).astype(jnp.bfloat16)[None][0]
    stream = residual.astype(jnp.float32) + row_norm(mixed.astype(jnp.float32), mixer_gain, 1e-06)
    normed_in = row_norm(stream, before_gain, 1e-06).astype(jnp.bfloat16)
    gathered = lax.all_gather(normed_in, "tp", axis=0, tiled=True)
    empty_hidden = jnp.zeros((gathered.shape[0], gate_weight.shape[1]), jnp.float32)
    pieces = (
        lax.all_gather(gate_weight, "sp", axis=0, tiled=True),
        lax.all_gather(up_weight, "sp", axis=0, tiled=True),
    )
    columns = lax.slice_in_dim(gathered, 0, pieces[0].shape[0], axis=1)
    gate_part = jnp.dot(columns, pieces[0], preferred_element_type=jnp.float32)
    up_part = jnp.dot(columns, pieces[1], preferred_element_type=jnp.float32)
    gate = empty_hidden + gate_part
    up = empty_hidden + up_part
    down_whole = lax.all_gather(down_weight, "sp", axis=1, tiled=True)
    hidden = (jax.nn.silu(gate) * up).astype(jnp.bfloat16)
    picked = lax.slice_in_dim(hidden, 0, lax.axis_size("tp") * quarter, axis=0)
    channel = lax.psum_scatter(
        jnp.dot(picked, down_whole, preferred_element_type=jnp.float32).astype(jnp.bfloat16),
        "tp",
        scatter_dimension=0,
        tiled=True,
    )
    updated = stream + 0.5 * row_norm(channel.astype(jnp.float32), after_gain, 1e-06)
    return updated.astype(jnp.bfloat16)


MESH = pl.DeviceIdType.MESH


def flip(index, bits):
    bit = 1
    while bit <= bits:
        if bits & bit:
            index = index + bit - 2 * bit * ((index // bit) % 2)
        bit *= 2
    return index


def layer(
    residual,
    queries,
    pair,
    lambdas,
    head_gain,
    out_weight,
    mixer_gain,
    before_gain,
    after_gain,
    gate_in,
    up_in,
    down_in,
    updated,
    kv,
    gate_w,
    up_w,
    down_w,
    head_out,
    head_in,
    stream,
    x,
    p,
    from_core,
    from_y,
    from_z,
    send_sems,
    recv_sems,
    local_sems,
):
    depth = gate_in.shape[0]
    n_tp = head_in.shape[0]
    quarter, width_all = residual.shape
    width = 2 * HEAD_DIM
    heads = queries.shape[1] // width
    place, member = lax.axis_index("sp"), lax.axis_index("tp")
    used = [0]
    copies = []

    def send(src, dst, axis, bits):
        at = used[0]
        used[0] += 1
        target = flip(place if axis == "sp" else member, bits)
        copy = pltpu.make_async_remote_copy(
            src_ref=src,
            dst_ref=dst,
            send_sem=send_sems.at[at],
            recv_sem=recv_sems.at[at],
            device_id={axis: target},
            device_id_type=MESH,
        )
        copy.start()
        copies.append(copy)
        return copy

    partners = [("sp", 1)] + [("sp", 2 * j) for j in range(1, depth)]
    partners += [("tp", j) for j in range(1, n_tp)]
    barrier = pltpu.get_barrier_semaphore()
    for axis, bits in partners:
        target = flip(place if axis == "sp" else member, bits)
        pl.semaphore_signal(barrier, inc=1, device_id={axis: target}, device_id_type=MESH)
    pl.semaphore_wait(barrier, len(partners))

    kv_z = [send(pair, kv.at[j], "sp", 2 * j) for j in range(1, depth)]
    kv_x = [send(pair, kv.at[depth], "sp", 1)]

    def scatter(source, target, at):
        mine = source.at[place // 2]
        local = pltpu.make_async_copy(mine, target.at[place], local_sems.at[at])
        local.start()
        over_z = [
            send(source.at[flip(place, 2 * j) // 2], target.at[place], "sp", 2 * j)
            for j in range(1, depth)
        ]
        return local, over_z, send(mine, target.at[place], "sp", 1)

    def forward(target, over_z):
        over_x = []
        for j in range(1, depth):
            over_z[j - 1].wait_recv()
            slot = target.at[flip(place, 2 * j)]
            over_x.append(send(slot, slot, "sp", 1))
        return over_x

    gate_moves = scatter(gate_in, gate_w, 0)
    up_moves = scatter(up_in, up_w, 1)
    kv[0] = pair[...]
    for j in range(1, depth):
        kv_z[j - 1].wait_recv()
        kv_x.append(send(kv.at[j], kv.at[depth + j], "sp", 1))
    for copy in kv_x:
        copy.wait_recv()

    def attend(tile, _):
        rows = pl.ds(pl.multiple_of(tile * quarter, quarter), quarter)
        for h in range(heads):
            parts = []
            for which in range(2):
                start = (2 * h + which) * HEAD_DIM
                query = queries[rows, start : start + HEAD_DIM]
                keys = kv[:, :, which * HEAD_DIM : (which + 1) * HEAD_DIM]
                keys = keys.reshape(2 * depth * keys.shape[1], HEAD_DIM)
                score = lax.dot_general(
                    query, keys, (((1,), (1,)), ((), ())), preferred_element_type=jnp.float32
                ) * (1.0 / math.sqrt(HEAD_DIM))
                expo = jnp.exp(score - jnp.max(score, axis=1, keepdims=True))
                total = jnp.sum(expo, axis=1, keepdims=True)
                vals = kv[:, :, width : 2 * width]
                vals = vals.reshape(2 * depth * vals.shape[1], width)
                numer = jnp.dot(
                    expo.astype(jnp.bfloat16), vals, preferred_element_type=jnp.float32
                )
                parts.append(numer / total)
            attended = parts[0] - lambdas[h] * parts[1]
            normed = row_norm(attended, head_gain[...], 1e-05).astype(jnp.bfloat16)
            head_out[tile, :, h * width : (h + 1) * width] = normed
        return 0

    lax.fori_loop(0, n_tp, attend, 0)
    moved = [send(head_out.at[flip(member, j)], head_in.at[member], "tp", j) for j in range(1, n_tp)]
    head_in[member] = head_out[member]
    gate_x = forward(gate_w, gate_moves[1])
    for copy in moved:
        copy.wait_recv()
    step = head_in.shape[2]
    mixed = jnp.zeros((quarter, width_all), jnp.float32)
    for m in range(n_tp):
        mixed = mixed + jnp.dot(
            head_in[m], out_weight[m * step : (m + 1) * step], preferred_element_type=jnp.float32
        )
    mixed = mixed.astype(jnp.bfloat16).astype(jnp.float32)
    stream[...] = residual[...].astype(jnp.float32) + row_norm(mixed, mixer_gain[...], 1e-06)
    x[0] = row_norm(stream[...], before_gain[...], 1e-06).astype(jnp.bfloat16)

    half = 2 * depth
    x_c = [send(x.at[0], x.at[half], "tp", 1)]
    x_z = [send(x.at[0], x.at[j], "sp", 2 * j) for j in range(1, depth)]
    x_y = [send(x.at[0], x.at[depth], "tp", 2)]
    down_moves = scatter(down_in, down_w, 2)
    up_x = forward(up_w, up_moves[1])
    for j in range(1, depth):
        x_z[j - 1].wait_recv()
        x_y.append(send(x.at[j], x.at[depth + j], "tp", 2))
        x_c.append(send(x.at[j], x.at[half + j], "tp", 1))
    x_last = []
    for j in range(depth):
        x_y[j].wait_recv()
        x_last.append(send(x.at[depth + j], x.at[half + depth + j], "tp", 1))
    down_x = forward(down_w, down_moves[1])

    for local, _, over_x in (gate_moves, up_moves, down_moves):
        local.wait()
        over_x.wait_recv()
    for copy in gate_x + up_x + down_x:
        copy.wait_recv()

    blocks = gate_w.shape[0]
    units = gate_w.shape[2]
    span = down_w.shape[2]

    def mix(tile, _):
        rows = x[pl.ds(2 * tile, 2)].reshape(2 * quarter, width_all)
        gate = jnp.dot(
            rows, gate_w[...].reshape(width_all, units), preferred_element_type=jnp.float32
        )
        up = jnp.dot(rows, up_w[...].reshape(width_all, units), preferred_element_type=jnp.float32)
        hidden = (gate / (1.0 + jnp.exp(-gate)) * up).astype(jnp.bfloat16)
        for m in range(blocks):
            part = jnp.dot(hidden, down_w[m], preferred_element_type=jnp.float32)
            p[pl.ds(2 * tile, 2), :, m * span : (m + 1) * span] = part.astype(
                jnp.bfloat16
            ).reshape(2, quarter, span)
        return 0

    def group(at):
        lax.fori_loop(at * depth // 2, (at + 1) * depth // 2, mix, 0)

    group(0)
    for copy in x_c:
        copy.wait_recv()
    group(2)
    r_c = [send(p.at[half + j], from_core.at[j], "tp", 1) for j in range(depth)]
    for copy in x_last:
        copy.wait_recv()
    group(3)
    r_d = [send(p.at[half + depth + j], from_core.at[depth + j], "tp", 1) for j in range(depth)]
    group(1)
    r_y = []
    order = list(range(1, depth)) + [0]
    for j in order:
        r_d[j].wait_recv()
        p[depth + j] = (
            p[depth + j].astype(jnp.float32) + from_core[depth + j].astype(jnp.float32)
        ).astype(jnp.bfloat16)
        r_y.append(send(p.at[depth + j], from_y.at[j], "tp", 2))
    r_z = []
    for i, j in enumerate(order):
        r_c[j].wait_recv()
        r_y[i].wait_recv()
        total = (
            p[j].astype(jnp.float32)
            + from_core[j].astype(jnp.float32)
            + from_y[j].astype(jnp.float32)
        )
        if j:
            p[j] = total.astype(jnp.bfloat16)
            r_z.append(send(p.at[j], from_z.at[j - 1], "sp", 2 * j))
    for j in range(1, depth):
        r_z[j - 1].wait_recv()
        total = total + from_z[j - 1].astype(jnp.float32)
    channel = total.astype(jnp.bfloat16).astype(jnp.float32)
    updated[...] = (stream[...] + 0.5 * row_norm(channel, after_gain[...], 1e-06)).astype(
        updated.dtype
    )
    for copy in copies:
        copy.wait_send()


def one_kernel(
    residual,
    queries,
    key_pairs,
    values,
    lambdas,
    head_gain,
    out_weight,
    mixer_gain,
    before_gain,
    after_gain,
    gate_weight,
    up_weight,
    down_weight,
):
    n_sp, n_tp = lax.axis_size("sp"), lax.axis_size("tp")
    depth = n_sp // 2
    quarter, width_all = residual.shape
    tokens_here, query_width = queries.shape
    inner, units_all = gate_weight.shape
    units = units_all // depth
    span = down_weight.shape[1]
    pair = jnp.concatenate([key_pairs, values], axis=1)
    gate_in = jnp.transpose(gate_weight.reshape(inner, depth, units), (1, 0, 2))
    up_in = jnp.transpose(up_weight.reshape(inner, depth, units), (1, 0, 2))
    down_in = down_weight.reshape(depth, units, span)
    tiles = 4 * depth
    total_sends = 7 * (depth - 1) + 4 + 3 + 3 * depth - 3 + n_tp - 1 + 2 * tiles
    vmem = pl.BlockSpec(memory_space=pltpu.VMEM)
    hbm = pl.BlockSpec(memory_space=pl.ANY)
    smem = pl.BlockSpec(memory_space=pltpu.SMEM)
    bf16 = jnp.bfloat16
    return pl.pallas_call(
        layer,
        out_shape=jax.ShapeDtypeStruct(residual.shape, bf16),
        in_specs=[vmem, vmem, vmem, smem] + [vmem] * 5 + [hbm] * 3,
        out_specs=vmem,
        scratch_shapes=[
            pltpu.VMEM((n_sp,) + pair.shape, bf16),
            pltpu.VMEM((n_sp, inner, units), bf16),
            pltpu.VMEM((n_sp, inner, units), bf16),
            pltpu.VMEM((n_sp, units, span), bf16),
            pltpu.VMEM((n_tp, quarter, query_width), bf16),
            pltpu.VMEM((n_tp, quarter, query_width), bf16),
            pltpu.VMEM((quarter, width_all), jnp.float32),
            pltpu.VMEM((tiles, quarter, width_all), bf16),
            pltpu.VMEM((tiles, quarter, width_all), bf16),
            pltpu.VMEM((2 * depth, quarter, width_all), bf16),
            pltpu.VMEM((depth, quarter, width_all), bf16),
            pltpu.VMEM((depth - 1, quarter, width_all), bf16),
            pltpu.SemaphoreType.DMA((total_sends,)),
            pltpu.SemaphoreType.DMA((total_sends,)),
            pltpu.SemaphoreType.DMA((3,)),
        ],
        compiler_params=pltpu.CompilerParams(
            collective_id=0, has_side_effects=True, vmem_limit_bytes=60 * 1024 * 1024
        ),
    )(
        residual,
        queries,
        pair,
        lambdas,
        head_gain[None],
        out_weight,
        mixer_gain[None],
        before_gain[None],
        after_gain[None],
        gate_in,
        up_in,
        down_in,
    )


def fits(mesh):
    return mesh.shape["tp"] == 4 and mesh.shape["sp"] == 8


def solution(mesh):
    return jax.shard_map(
        one_kernel if fits(mesh) else on_device,
        mesh=mesh,
        in_specs=(
            P(("sp", "tp"), None),
            P("sp", "tp"),
            P("sp", "tp"),
            P("sp", "tp"),
            P("tp"),
            P(),
            P(),
            P(),
            P(),
            P(),
            P("sp", "tp"),
            P("sp", "tp"),
            P("tp", "sp"),
        ),
        out_specs=P(("sp", "tp"), None),
        check_vma=False,
    )
```

```python
import math

import jax
import jax.numpy as jnp
from jax import lax
from jax.experimental import pallas as pl
from jax.experimental.pallas import tpu as pltpu
from jax.sharding import PartitionSpec as P

HEAD_DIM = 64


def row_norm(values_in, gain, epsilon):
    mean_square = jnp.mean(values_in * values_in, axis=-1, keepdims=True)
    return values_in * lax.rsqrt(mean_square + epsilon) * gain


def on_device(
    residual,
    queries,
    key_pairs,
    values,
    lambdas,
    head_gain,
    out_weight,
    mixer_gain,
    before_gain,
    after_gain,
    gate_weight,
    up_weight,
    down_weight,
):
    tokens_here = queries.shape[0]
    quarter = residual.shape[0]
    width = 2 * HEAD_DIM
    local_heads = queries.shape[1] // width
    scale = 1.0 / math.sqrt(HEAD_DIM)
    height = local_heads * tokens_here
    query_rows = jnp.transpose(
        queries.reshape(tokens_here, local_heads, 2, HEAD_DIM), (2, 1, 0, 3)
    ).reshape(2, height, HEAD_DIM)
    empty = (
        jnp.full((height,), -1e30, jnp.float32),
        jnp.zeros((height,), jnp.float32),
        jnp.zeros((height, width), jnp.float32),
    )
    state = (empty, empty)
    key_piece = lax.all_gather(key_pairs, "sp", axis=0, tiled=True)
    value_piece = lax.all_gather(values, "sp", axis=0, tiled=True)
    length = key_piece.shape[0]
    span = length
    for split_count in range(1, length + 1):
        if length % split_count == 0 and length // split_count <= 2048:
            span = length // split_count
            break
    key_blocks = key_piece.reshape(length // span, span, 2, HEAD_DIM)
    value_blocks = value_piece.reshape(length // span, span, width)

    def advance(carry, blocks_in):
        key_block, value_block = blocks_in
        renewed = []
        for which in range(2):
            running_top, running_total, running_numer = carry[which]
            score = (
                jnp.dot(
                    query_rows[which], key_block[:, which].T, preferred_element_type=jnp.float32
                )
                * scale
            )
            new_top = jnp.maximum(running_top, jnp.max(score, axis=1))
            shrink = jnp.exp(running_top - new_top)
            expo = jnp.exp(score - new_top[:, None])
            new_total = running_total * shrink + jnp.sum(expo, axis=1)
            new_numer = running_numer * shrink[:, None] + jnp.dot(
                expo.astype(jnp.bfloat16), value_block, preferred_element_type=jnp.float32
            )
            renewed.append((new_top, new_total, new_numer))
        return (tuple(renewed), None)

    state, _ = lax.scan(advance, state, (key_blocks, value_blocks))
    first_map, second_map = state
    lambda_rows = jnp.repeat(lambdas, tokens_here)[:, None]
    attended = first_map[2] / first_map[1][:, None] - lambda_rows * (
        second_map[2] / second_map[1][:, None]
    )
    normed = row_norm(attended, head_gain, 1e-05).astype(jnp.bfloat16)
    head_out = jnp.transpose(normed.reshape(local_heads, tokens_here, width), (1, 0, 2)).reshape(
        tokens_here, local_heads * width
    )
    grouped = head_out.reshape(lax.axis_size("tp"), quarter, local_heads * width)
    mixed = jnp.dot(
        lax.all_to_all(grouped, "tp", split_axis=0, concat_axis=2, tiled=True)[0],
        out_weight,
        preferred_element_type=jnp.float32,
    ).astype(jnp.bfloat16)[None][0]
    stream = residual.astype(jnp.float32) + row_norm(mixed.astype(jnp.float32), mixer_gain, 1e-06)
    normed_in = row_norm(stream, before_gain, 1e-06).astype(jnp.bfloat16)
    gathered = lax.all_gather(normed_in, "tp", axis=0, tiled=True)
    empty_hidden = jnp.zeros((gathered.shape[0], gate_weight.shape[1]), jnp.float32)
    pieces = (
        lax.all_gather(gate_weight, "sp", axis=0, tiled=True),
        lax.all_gather(up_weight, "sp", axis=0, tiled=True),
    )
    columns = lax.slice_in_dim(gathered, 0, pieces[0].shape[0], axis=1)
    gate_part = jnp.dot(columns, pieces[0], preferred_element_type=jnp.float32)
    up_part = jnp.dot(columns, pieces[1], preferred_element_type=jnp.float32)
    gate = empty_hidden + gate_part
    up = empty_hidden + up_part
    down_whole = lax.all_gather(down_weight, "sp", axis=1, tiled=True)
    hidden = (jax.nn.silu(gate) * up).astype(jnp.bfloat16)
    picked = lax.slice_in_dim(hidden, 0, lax.axis_size("tp") * quarter, axis=0)
    channel = lax.psum_scatter(
        jnp.dot(picked, down_whole, preferred_element_type=jnp.float32).astype(jnp.bfloat16),
        "tp",
        scatter_dimension=0,
        tiled=True,
    )
    updated = stream + 0.5 * row_norm(channel.astype(jnp.float32), after_gain, 1e-06)
    return updated.astype(jnp.bfloat16)


MESH = pl.DeviceIdType.MESH


def flip(index, bits):
    bit = 1
    while bit <= bits:
        if bits & bit:
            index = index + bit - 2 * bit * ((index // bit) % 2)
        bit *= 2
    return index


def layer(
    residual,
    queries,
    key_pairs,
    values,
    lambdas,
    head_gain,
    out_weight,
    mixer_gain,
    before_gain,
    after_gain,
    gate_weight,
    up_weight,
    down_in,
    updated,
    gate_in,
    up_in,
    hidden,
    kv,
    gate_w,
    up_w,
    down_w,
    head_out,
    head_in,
    stream,
    x,
    p,
    from_core,
    from_y,
    from_z,
    send_sems,
    recv_sems,
    local_sems,
):
    depth = down_in.shape[0]
    n_tp = head_in.shape[0]
    quarter, width_all = residual.shape
    width = 2 * HEAD_DIM
    heads = queries.shape[1] // width
    place, member = lax.axis_index("sp"), lax.axis_index("tp")
    used = [0]
    copies = []

    def send(src, dst, axis, bits):
        at = used[0]
        used[0] += 1
        target = flip(place if axis == "sp" else member, bits)
        copy = pltpu.make_async_remote_copy(
            src_ref=src,
            dst_ref=dst,
            send_sem=send_sems.at[at],
            recv_sem=recv_sems.at[at],
            device_id={axis: target},
            device_id_type=MESH,
        )
        copy.start()
        copies.append(copy)
        return copy

    partners = [("sp", 1)] + [("sp", 2 * j) for j in range(1, depth)]
    partners += [("tp", j) for j in range(1, n_tp)]
    barrier = pltpu.get_barrier_semaphore()
    for axis, bits in partners:
        target = flip(place if axis == "sp" else member, bits)
        pl.semaphore_signal(barrier, inc=1, device_id={axis: target}, device_id_type=MESH)
    pl.semaphore_wait(barrier, len(partners))

    kv[0, :, :width] = key_pairs[...]
    kv[0, :, width:] = values[...]
    far = send(kv.at[0], kv.at[2], "sp", 4)
    near = send(kv.at[0], kv.at[1], "sp", 2)
    kv_x = [send(kv.at[0], kv.at[depth], "sp", 1)]
    for source, target in ((gate_weight, gate_in), (up_weight, up_in)):
        columns = target.shape[2]
        for j in range(depth):
            target[j] = source[:, j * columns : (j + 1) * columns]
    far.wait_recv()
    relayed = send(kv.at[2], kv.at[3], "sp", 2)
    kv_x.append(send(kv.at[2], kv.at[depth + 2], "sp", 1))

    def scatter(source, target, at):
        mine = source.at[place // 2]
        local = pltpu.make_async_copy(mine, target.at[place], local_sems.at[at])
        local.start()
        over_z = [
            send(source.at[flip(place, 2 * j) // 2], target.at[place], "sp", 2 * j)
            for j in range(1, depth)
        ]
        return local, over_z, send(mine, target.at[place], "sp", 1)

    def forward(target, over_z):
        over_x = []
        for j in range(1, depth):
            over_z[j - 1].wait_recv()
            slot = target.at[flip(place, 2 * j)]
            over_x.append(send(slot, slot, "sp", 1))
        return over_x

    gate_moves = scatter(gate_in, gate_w, 0)
    up_moves = scatter(up_in, up_w, 1)
    for j, copy in ((1, near), (3, relayed)):
        copy.wait_recv()
        kv_x.append(send(kv.at[j], kv.at[depth + j], "sp", 1))
    for copy in kv_x:
        copy.wait_recv()

    def attend(tile, _):
        rows = pl.ds(pl.multiple_of(tile * quarter, quarter), quarter)
        for h in range(heads):
            parts = []
            for which in range(2):
                start = (2 * h + which) * HEAD_DIM
                query = queries[rows, start : start + HEAD_DIM]
                keys = kv[:, :, which * HEAD_DIM : (which + 1) * HEAD_DIM]
                keys = keys.reshape(2 * depth * keys.shape[1], HEAD_DIM)
                score = lax.dot_general(
                    query, keys, (((1,), (1,)), ((), ())), preferred_element_type=jnp.float32
                ) * (1.0 / math.sqrt(HEAD_DIM))
                expo = jnp.exp(score - jnp.max(score, axis=1, keepdims=True))
                total = jnp.sum(expo, axis=1, keepdims=True)
                vals = kv[:, :, width : 2 * width]
                vals = vals.reshape(2 * depth * vals.shape[1], width)
                numer = jnp.dot(
                    expo.astype(jnp.bfloat16), vals, preferred_element_type=jnp.float32
                )
                parts.append(numer / total)
            attended = parts[0] - lambdas[h] * parts[1]
            normed = row_norm(attended, head_gain[...], 1e-05).astype(jnp.bfloat16)
            head_out[tile, :, h * width : (h + 1) * width] = normed
        return 0

    lax.fori_loop(0, n_tp, attend, 0)
    moved = [send(head_out.at[flip(member, j)], head_in.at[member], "tp", j) for j in range(1, n_tp)]
    head_in[member] = head_out[member]
    gate_x = forward(gate_w, gate_moves[1])
    for copy in moved:
        copy.wait_recv()
    step = head_in.shape[2]
    mixed = jnp.zeros((quarter, width_all), jnp.float32)
    for m in range(n_tp):
        mixed = mixed + jnp.dot(
            head_in[m], out_weight[m * step : (m + 1) * step], preferred_element_type=jnp.float32
        )
    mixed = mixed.astype(jnp.bfloat16).astype(jnp.float32)
    stream[...] = residual[...].astype(jnp.float32) + row_norm(mixed, mixer_gain[...], 1e-06)
    x[0] = row_norm(stream[...], before_gain[...], 1e-06).astype(jnp.bfloat16)

    half = 2 * depth
    far = send(x.at[0], x.at[2], "sp", 4)
    near = send(x.at[0], x.at[1], "sp", 2)
    x_c = [send(x.at[0], x.at[half], "tp", 1)]
    x_y = [send(x.at[0], x.at[depth], "tp", 2)]
    up_x = forward(up_w, up_moves[1])
    far.wait_recv()
    relayed = send(x.at[2], x.at[3], "sp", 2)
    down_moves = scatter(down_in, down_w, 2)
    order = ((2, far), (1, near), (3, relayed))
    for j, copy in order:
        if j != 2:
            copy.wait_recv()
        x_y.append(send(x.at[j], x.at[depth + j], "tp", 2))
        x_c.append(send(x.at[j], x.at[half + j], "tp", 1))
    for local, _, over_x in (gate_moves, up_moves):
        local.wait()
        over_x.wait_recv()
    for copy in gate_x + up_x:
        copy.wait_recv()

    blocks = gate_w.shape[0]
    units = gate_w.shape[2]
    span = down_w.shape[2]

    def widen(tile, _):
        rows = x[pl.ds(2 * tile, 2)].reshape(2 * quarter, width_all)
        gate = jnp.dot(
            rows, gate_w[...].reshape(width_all, units), preferred_element_type=jnp.float32
        )
        up = jnp.dot(rows, up_w[...].reshape(width_all, units), preferred_element_type=jnp.float32)
        hidden[tile] = (gate / (1.0 + jnp.exp(-gate)) * up).astype(jnp.bfloat16)
        return 0

    def narrow(tile, _):
        for m in range(blocks):
            part = jnp.dot(hidden[tile], down_w[m], preferred_element_type=jnp.float32)
            p[pl.ds(2 * tile, 2), :, m * span : (m + 1) * span] = part.astype(
                jnp.bfloat16
            ).reshape(2, quarter, span)
        return 0

    def group(at, body):
        lax.fori_loop(at * depth // 2, (at + 1) * depth // 2, body, 0)

    group(0, widen)
    x_last = []
    for j, copy in zip((0, 2, 1, 3), x_y):
        copy.wait_recv()
        x_last.append(send(x.at[depth + j], x.at[half + depth + j], "tp", 1))
    down_x = forward(down_w, down_moves[1])
    for copy in x_c:
        copy.wait_recv()
    group(2, widen)
    group(1, widen)
    for copy in x_last:
        copy.wait_recv()
    group(3, widen)
    down_moves[0].wait()
    down_moves[2].wait_recv()
    for copy in down_x:
        copy.wait_recv()
    group(3, narrow)
    r_d = [send(p.at[half + depth + j], from_core.at[depth + j], "tp", 1) for j in range(depth)]
    group(1, narrow)
    r_y = []
    turns = (3, 1, 2, 0)
    for j in turns:
        r_d[j].wait_recv()
        p[depth + j] = (
            p[depth + j].astype(jnp.float32) + from_core[depth + j].astype(jnp.float32)
        ).astype(jnp.bfloat16)
        r_y.append(send(p.at[depth + j], from_y.at[j], "tp", 2))
    group(2, narrow)
    r_c = [send(p.at[half + j], from_core.at[j], "tp", 1) for j in range(depth)]
    group(0, narrow)
    r_z = []
    for copy, j in zip(r_y, turns):
        r_c[j].wait_recv()
        copy.wait_recv()
        total = (
            p[j].astype(jnp.float32)
            + from_core[j].astype(jnp.float32)
            + from_y[j].astype(jnp.float32)
        )
        if j == 2:
            r_z[0].wait_recv()
            total = total + from_z[2].astype(jnp.float32)
        if j:
            p[j] = total.astype(jnp.bfloat16)
            r_z.append(send(p.at[j], from_z.at[j - 1], "sp", 4 if j == 2 else 2))
    for copy, slot in ((r_z[1], 0), (r_z[2], 1)):
        copy.wait_recv()
        total = total + from_z[slot].astype(jnp.float32)
    channel = total.astype(jnp.bfloat16).astype(jnp.float32)
    updated[...] = (stream[...] + 0.5 * row_norm(channel, after_gain[...], 1e-06)).astype(
        updated.dtype
    )
    for copy in copies:
        copy.wait_send()


def one_kernel(
    residual,
    queries,
    key_pairs,
    values,
    lambdas,
    head_gain,
    out_weight,
    mixer_gain,
    before_gain,
    after_gain,
    gate_weight,
    up_weight,
    down_weight,
):
    n_sp, n_tp = lax.axis_size("sp"), lax.axis_size("tp")
    depth = n_sp // 2
    quarter, width_all = residual.shape
    tokens_here, query_width = queries.shape
    inner, units_all = gate_weight.shape
    units = units_all // depth
    span = down_weight.shape[1]
    down_in = down_weight.reshape(depth, units, span)
    tiles = 4 * depth
    total_sends = 7 * (depth - 1) + 4 + 3 + 3 * depth - 3 + n_tp - 1 + 2 * tiles
    vmem = pl.BlockSpec(memory_space=pltpu.VMEM)
    hbm = pl.BlockSpec(memory_space=pl.ANY)
    smem = pl.BlockSpec(memory_space=pltpu.SMEM)
    bf16 = jnp.bfloat16
    return pl.pallas_call(
        layer,
        out_shape=jax.ShapeDtypeStruct(residual.shape, bf16),
        in_specs=[vmem] * 4 + [smem] + [vmem] * 7 + [hbm],
        out_specs=vmem,
        scratch_shapes=[
            pltpu.VMEM((depth, inner, units), bf16),
            pltpu.VMEM((depth, inner, units), bf16),
            pltpu.VMEM((tiles // 2, 2 * quarter, units), bf16),
            pltpu.VMEM((n_sp, tokens_here, 2 * key_pairs.shape[1]), bf16),
            pltpu.VMEM((n_sp, inner, units), bf16),
            pltpu.VMEM((n_sp, inner, units), bf16),
            pltpu.VMEM((n_sp, units, span), bf16),
            pltpu.VMEM((n_tp, quarter, query_width), bf16),
            pltpu.VMEM((n_tp, quarter, query_width), bf16),
            pltpu.VMEM((quarter, width_all), jnp.float32),
            pltpu.VMEM((tiles, quarter, width_all), bf16),
            pltpu.VMEM((tiles, quarter, width_all), bf16),
            pltpu.VMEM((2 * depth, quarter, width_all), bf16),
            pltpu.VMEM((depth, quarter, width_all), bf16),
            pltpu.VMEM((depth - 1, quarter, width_all), bf16),
            pltpu.SemaphoreType.DMA((total_sends,)),
            pltpu.SemaphoreType.DMA((total_sends,)),
            pltpu.SemaphoreType.DMA((3,)),
        ],
        compiler_params=pltpu.CompilerParams(
            collective_id=0, has_side_effects=True, vmem_limit_bytes=60 * 1024 * 1024
        ),
    )(
        residual,
        queries,
        key_pairs,
        values,
        lambdas,
        head_gain[None],
        out_weight,
        mixer_gain[None],
        before_gain[None],
        after_gain[None],
        gate_weight,
        up_weight,
        down_in,
    )


def fits(mesh):
    return mesh.shape["tp"] == 4 and mesh.shape["sp"] == 8


def solution(mesh):
    return jax.shard_map(
        one_kernel if fits(mesh) else on_device,
        mesh=mesh,
        in_specs=(
            P(("sp", "tp"), None),
            P("sp", "tp"),
            P("sp", "tp"),
            P("sp", "tp"),
            P("tp"),
            P(),
            P(),
            P(),
            P(),
            P(),
            P("sp", "tp"),
            P("sp", "tp"),
            P("tp", "sp"),
        ),
        out_specs=P(("sp", "tp"), None),
        check_vma=False,
    )
```

```python
import math

import jax
import jax.numpy as jnp
from jax import lax
from jax.experimental import pallas as pl
from jax.experimental.pallas import tpu as pltpu
from jax.sharding import PartitionSpec as P

HEAD_DIM = 64


def row_norm(values_in, gain, epsilon):
    mean_square = jnp.mean(values_in * values_in, axis=-1, keepdims=True)
    return values_in * lax.rsqrt(mean_square + epsilon) * gain


def on_device(
    residual,
    queries,
    key_pairs,
    values,
    lambdas,
    head_gain,
    out_weight,
    mixer_gain,
    before_gain,
    after_gain,
    gate_weight,
    up_weight,
    down_weight,
):
    tokens_here = queries.shape[0]
    quarter = residual.shape[0]
    width = 2 * HEAD_DIM
    local_heads = queries.shape[1] // width
    scale = 1.0 / math.sqrt(HEAD_DIM)
    height = local_heads * tokens_here
    query_rows = jnp.transpose(
        queries.reshape(tokens_here, local_heads, 2, HEAD_DIM), (2, 1, 0, 3)
    ).reshape(2, height, HEAD_DIM)
    empty = (
        jnp.full((height,), -1e30, jnp.float32),
        jnp.zeros((height,), jnp.float32),
        jnp.zeros((height, width), jnp.float32),
    )
    state = (empty, empty)
    key_piece = lax.all_gather(key_pairs, "sp", axis=0, tiled=True)
    value_piece = lax.all_gather(values, "sp", axis=0, tiled=True)
    length = key_piece.shape[0]
    span = length
    for split_count in range(1, length + 1):
        if length % split_count == 0 and length // split_count <= 2048:
            span = length // split_count
            break
    key_blocks = key_piece.reshape(length // span, span, 2, HEAD_DIM)
    value_blocks = value_piece.reshape(length // span, span, width)

    def advance(carry, blocks_in):
        key_block, value_block = blocks_in
        renewed = []
        for which in range(2):
            running_top, running_total, running_numer = carry[which]
            score = (
                jnp.dot(
                    query_rows[which], key_block[:, which].T, preferred_element_type=jnp.float32
                )
                * scale
            )
            new_top = jnp.maximum(running_top, jnp.max(score, axis=1))
            shrink = jnp.exp(running_top - new_top)
            expo = jnp.exp(score - new_top[:, None])
            new_total = running_total * shrink + jnp.sum(expo, axis=1)
            new_numer = running_numer * shrink[:, None] + jnp.dot(
                expo.astype(jnp.bfloat16), value_block, preferred_element_type=jnp.float32
            )
            renewed.append((new_top, new_total, new_numer))
        return (tuple(renewed), None)

    state, _ = lax.scan(advance, state, (key_blocks, value_blocks))
    first_map, second_map = state
    lambda_rows = jnp.repeat(lambdas, tokens_here)[:, None]
    attended = first_map[2] / first_map[1][:, None] - lambda_rows * (
        second_map[2] / second_map[1][:, None]
    )
    normed = row_norm(attended, head_gain, 1e-05).astype(jnp.bfloat16)
    head_out = jnp.transpose(normed.reshape(local_heads, tokens_here, width), (1, 0, 2)).reshape(
        tokens_here, local_heads * width
    )
    grouped = head_out.reshape(lax.axis_size("tp"), quarter, local_heads * width)
    mixed = jnp.dot(
        lax.all_to_all(grouped, "tp", split_axis=0, concat_axis=2, tiled=True)[0],
        out_weight,
        preferred_element_type=jnp.float32,
    ).astype(jnp.bfloat16)[None][0]
    stream = residual.astype(jnp.float32) + row_norm(mixed.astype(jnp.float32), mixer_gain, 1e-06)
    normed_in = row_norm(stream, before_gain, 1e-06).astype(jnp.bfloat16)
    gathered = lax.all_gather(normed_in, "tp", axis=0, tiled=True)
    empty_hidden = jnp.zeros((gathered.shape[0], gate_weight.shape[1]), jnp.float32)
    pieces = (
        lax.all_gather(gate_weight, "sp", axis=0, tiled=True),
        lax.all_gather(up_weight, "sp", axis=0, tiled=True),
    )
    columns = lax.slice_in_dim(gathered, 0, pieces[0].shape[0], axis=1)
    gate_part = jnp.dot(columns, pieces[0], preferred_element_type=jnp.float32)
    up_part = jnp.dot(columns, pieces[1], preferred_element_type=jnp.float32)
    gate = empty_hidden + gate_part
    up = empty_hidden + up_part
    down_whole = lax.all_gather(down_weight, "sp", axis=1, tiled=True)
    hidden = (jax.nn.silu(gate) * up).astype(jnp.bfloat16)
    picked = lax.slice_in_dim(hidden, 0, lax.axis_size("tp") * quarter, axis=0)
    channel = lax.psum_scatter(
        jnp.dot(picked, down_whole, preferred_element_type=jnp.float32).astype(jnp.bfloat16),
        "tp",
        scatter_dimension=0,
        tiled=True,
    )
    updated = stream + 0.5 * row_norm(channel.astype(jnp.float32), after_gain, 1e-06)
    return updated.astype(jnp.bfloat16)


MESH = pl.DeviceIdType.MESH


def flip(index, bits):
    bit = 1
    while bit <= bits:
        if bits & bit:
            index = index + bit - 2 * bit * ((index // bit) % 2)
        bit *= 2
    return index


def layer(
    residual,
    queries,
    key_pairs,
    values,
    lambdas,
    head_gain,
    out_weight,
    mixer_gain,
    before_gain,
    after_gain,
    gate_weight,
    up_weight,
    down_in,
    updated,
    gate_in,
    up_in,
    hidden,
    kv,
    gate_w,
    up_w,
    down_w,
    head_out,
    head_in,
    stream,
    x,
    p,
    from_core,
    from_y,
    from_z,
    send_sems,
    recv_sems,
    local_sems,
):
    depth = down_in.shape[0]
    n_tp = head_in.shape[0]
    quarter, width_all = residual.shape
    width = 2 * HEAD_DIM
    heads = queries.shape[1] // width
    place, member = lax.axis_index("sp"), lax.axis_index("tp")
    used = [0]
    copies = []

    def send(src, dst, axis, bits):
        at = used[0]
        used[0] += 1
        target = flip(place if axis == "sp" else member, bits)
        copy = pltpu.make_async_remote_copy(
            src_ref=src,
            dst_ref=dst,
            send_sem=send_sems.at[at],
            recv_sem=recv_sems.at[at],
            device_id={axis: target},
            device_id_type=MESH,
        )
        copy.start()
        copies.append(copy)
        return copy

    partners = [("sp", 1)] + [("sp", 2 * j) for j in range(1, depth)]
    partners += [("tp", j) for j in range(1, n_tp)]
    barrier = pltpu.get_barrier_semaphore()
    for axis, bits in partners:
        target = flip(place if axis == "sp" else member, bits)
        pl.semaphore_signal(barrier, inc=1, device_id={axis: target}, device_id_type=MESH)
    pl.semaphore_wait(barrier, len(partners))

    kv[0, :, :width] = key_pairs[...]
    kv[0, :, width:] = values[...]
    far = send(kv.at[0], kv.at[2], "sp", 4)
    near = send(kv.at[0], kv.at[1], "sp", 2)
    kv_x = [send(kv.at[0], kv.at[depth], "sp", 1)]
    for source, target in ((gate_weight, gate_in), (up_weight, up_in)):
        columns = target.shape[2]
        for j in range(depth):
            target[j] = source[:, j * columns : (j + 1) * columns]
    far.wait_recv()
    relayed = send(kv.at[2], kv.at[3], "sp", 2)
    kv_x.append(send(kv.at[2], kv.at[depth + 2], "sp", 1))

    def scatter(source, target, at):
        mine = source.at[place // 2]
        local = pltpu.make_async_copy(mine, target.at[place], local_sems.at[at])
        local.start()
        over_z = [
            send(source.at[flip(place, 2 * j) // 2], target.at[place], "sp", 2 * j)
            for j in range(1, depth)
        ]
        return local, over_z, send(mine, target.at[place], "sp", 1)

    def forward(target, over_z):
        over_x = []
        for j in range(1, depth):
            over_z[j - 1].wait_recv()
            slot = target.at[flip(place, 2 * j)]
            over_x.append(send(slot, slot, "sp", 1))
        return over_x

    gate_moves = scatter(gate_in, gate_w, 0)
    up_moves = scatter(up_in, up_w, 1)
    down_local = pltpu.make_async_copy(down_in.at[place // 2], down_w.at[place], local_sems.at[2])
    down_local.start()
    down_x = [send(down_in.at[place // 2], down_w.at[place], "sp", 1)]
    for j, copy in ((1, near), (3, relayed)):
        copy.wait_recv()
        kv_x.append(send(kv.at[j], kv.at[depth + j], "sp", 1))
    for copy in kv_x:
        copy.wait_recv()

    def attend(tile, _):
        rows = pl.ds(pl.multiple_of(tile * quarter, quarter), quarter)
        for h in range(heads):
            parts = []
            for which in range(2):
                start = (2 * h + which) * HEAD_DIM
                query = queries[rows, start : start + HEAD_DIM]
                keys = kv[:, :, which * HEAD_DIM : (which + 1) * HEAD_DIM]
                keys = keys.reshape(2 * depth * keys.shape[1], HEAD_DIM)
                score = lax.dot_general(
                    query, keys, (((1,), (1,)), ((), ())), preferred_element_type=jnp.float32
                ) * (1.0 / math.sqrt(HEAD_DIM))
                expo = jnp.exp(score - jnp.max(score, axis=1, keepdims=True))
                total = jnp.sum(expo, axis=1, keepdims=True)
                vals = kv[:, :, width : 2 * width]
                vals = vals.reshape(2 * depth * vals.shape[1], width)
                numer = jnp.dot(
                    expo.astype(jnp.bfloat16), vals, preferred_element_type=jnp.float32
                )
                parts.append(numer / total)
            attended = parts[0] - lambdas[h] * parts[1]
            normed = row_norm(attended, head_gain[...], 1e-05).astype(jnp.bfloat16)
            head_out[tile, :, h * width : (h + 1) * width] = normed
        return 0

    lax.fori_loop(0, n_tp, attend, 0)
    moved = [send(head_out.at[flip(member, j)], head_in.at[member], "tp", j) for j in range(1, n_tp)]
    head_in[member] = head_out[member]
    gate_x = forward(gate_w, gate_moves[1])
    for copy in moved:
        copy.wait_recv()
    step = head_in.shape[2]
    mixed = jnp.zeros((quarter, width_all), jnp.float32)
    for m in range(n_tp):
        mixed = mixed + jnp.dot(
            head_in[m], out_weight[m * step : (m + 1) * step], preferred_element_type=jnp.float32
        )
    mixed = mixed.astype(jnp.bfloat16).astype(jnp.float32)
    stream[...] = residual[...].astype(jnp.float32) + row_norm(mixed, mixer_gain[...], 1e-06)
    x[0] = row_norm(stream[...], before_gain[...], 1e-06).astype(jnp.bfloat16)

    half = 2 * depth
    far = send(x.at[0], x.at[2], "sp", 4)
    near = send(x.at[0], x.at[1], "sp", 2)
    x_c = [send(x.at[0], x.at[half], "tp", 1)]
    x_y = [send(x.at[0], x.at[depth], "tp", 2)]
    up_x = forward(up_w, up_moves[1])
    far.wait_recv()
    relayed = send(x.at[2], x.at[3], "sp", 2)
    down_z = [
        send(down_in.at[flip(place, 2 * j) // 2], down_w.at[place], "sp", 2 * j)
        for j in range(1, depth)
    ]
    order = ((2, far), (1, near), (3, relayed))
    for j, copy in order:
        if j != 2:
            copy.wait_recv()
        x_y.append(send(x.at[j], x.at[depth + j], "tp", 2))
        x_c.append(send(x.at[j], x.at[half + j], "tp", 1))
    for local, _, over_x in (gate_moves, up_moves):
        local.wait()
        over_x.wait_recv()
    for copy in gate_x + up_x:
        copy.wait_recv()

    blocks = gate_w.shape[0]
    units = gate_w.shape[2]
    span = down_w.shape[2]

    def widen(tile, _):
        rows = x[pl.ds(2 * tile, 2)].reshape(2 * quarter, width_all)
        gate = jnp.dot(
            rows, gate_w[...].reshape(width_all, units), preferred_element_type=jnp.float32
        )
        up = jnp.dot(rows, up_w[...].reshape(width_all, units), preferred_element_type=jnp.float32)
        hidden[tile] = (gate / (1.0 + jnp.exp(-gate)) * up).astype(jnp.bfloat16)
        return 0

    def narrow(tile, _):
        for m in range(blocks):
            part = jnp.dot(hidden[tile], down_w[m], preferred_element_type=jnp.float32)
            p[pl.ds(2 * tile, 2), :, m * span : (m + 1) * span] = part.astype(
                jnp.bfloat16
            ).reshape(2, quarter, span)
        return 0

    def group(at, body):
        lax.fori_loop(at * depth // 2, (at + 1) * depth // 2, body, 0)

    group(0, widen)
    x_last = []
    for i, j in enumerate((0, 2, 1, 3)):
        if i:
            down_z[i - 1].wait_recv()
            slot = down_w.at[flip(place, 2 * i)]
            down_x.append(send(slot, slot, "sp", 1))
        x_y[i].wait_recv()
        x_last.append(send(x.at[depth + j], x.at[half + depth + j], "tp", 1))
    for copy in x_c:
        copy.wait_recv()
    group(2, widen)
    group(1, widen)
    for copy in x_last:
        copy.wait_recv()
    group(3, widen)
    down_local.wait()
    for copy in down_x:
        copy.wait_recv()
    group(3, narrow)
    r_d = [send(p.at[half + depth + j], from_core.at[depth + j], "tp", 1) for j in range(depth)]
    group(1, narrow)
    r_y = []
    turns = (3, 1, 2, 0)
    for j in turns:
        r_d[j].wait_recv()
        p[depth + j] = (
            p[depth + j].astype(jnp.float32) + from_core[depth + j].astype(jnp.float32)
        ).astype(jnp.bfloat16)
        r_y.append(send(p.at[depth + j], from_y.at[j], "tp", 2))
    group(2, narrow)
    r_c = [send(p.at[half + j], from_core.at[j], "tp", 1) for j in range(depth)]
    group(0, narrow)
    r_z = []
    for copy, j in zip(r_y, turns):
        r_c[j].wait_recv()
        copy.wait_recv()
        total = (
            p[j].astype(jnp.float32)
            + from_core[j].astype(jnp.float32)
            + from_y[j].astype(jnp.float32)
        )
        if j == 2:
            r_z[0].wait_recv()
            total = total + from_z[2].astype(jnp.float32)
        if j:
            p[j] = total.astype(jnp.bfloat16)
            r_z.append(send(p.at[j], from_z.at[j - 1], "sp", 4 if j == 2 else 2))
    for copy, slot in ((r_z[1], 0), (r_z[2], 1)):
        copy.wait_recv()
        total = total + from_z[slot].astype(jnp.float32)
    channel = total.astype(jnp.bfloat16).astype(jnp.float32)
    updated[...] = (stream[...] + 0.5 * row_norm(channel, after_gain[...], 1e-06)).astype(
        updated.dtype
    )
    for copy in copies:
        copy.wait_send()


def one_kernel(
    residual,
    queries,
    key_pairs,
    values,
    lambdas,
    head_gain,
    out_weight,
    mixer_gain,
    before_gain,
    after_gain,
    gate_weight,
    up_weight,
    down_weight,
):
    n_sp, n_tp = lax.axis_size("sp"), lax.axis_size("tp")
    depth = n_sp // 2
    quarter, width_all = residual.shape
    tokens_here, query_width = queries.shape
    inner, units_all = gate_weight.shape
    units = units_all // depth
    span = down_weight.shape[1]
    down_in = down_weight.reshape(depth, units, span)
    tiles = 4 * depth
    total_sends = 7 * (depth - 1) + 4 + 3 + 3 * depth - 3 + n_tp - 1 + 2 * tiles
    vmem = pl.BlockSpec(memory_space=pltpu.VMEM)
    hbm = pl.BlockSpec(memory_space=pl.ANY)
    smem = pl.BlockSpec(memory_space=pltpu.SMEM)
    bf16 = jnp.bfloat16
    return pl.pallas_call(
        layer,
        out_shape=jax.ShapeDtypeStruct(residual.shape, bf16),
        in_specs=[vmem] * 4 + [smem] + [vmem] * 7 + [hbm],
        out_specs=vmem,
        scratch_shapes=[
            pltpu.VMEM((depth, inner, units), bf16),
            pltpu.VMEM((depth, inner, units), bf16),
            pltpu.VMEM((tiles // 2, 2 * quarter, units), bf16),
            pltpu.VMEM((n_sp, tokens_here, 2 * key_pairs.shape[1]), bf16),
            pltpu.VMEM((n_sp, inner, units), bf16),
            pltpu.VMEM((n_sp, inner, units), bf16),
            pltpu.VMEM((n_sp, units, span), bf16),
            pltpu.VMEM((n_tp, quarter, query_width), bf16),
            pltpu.VMEM((n_tp, quarter, query_width), bf16),
            pltpu.VMEM((quarter, width_all), jnp.float32),
            pltpu.VMEM((tiles, quarter, width_all), bf16),
            pltpu.VMEM((tiles, quarter, width_all), bf16),
            pltpu.VMEM((2 * depth, quarter, width_all), bf16),
            pltpu.VMEM((depth, quarter, width_all), bf16),
            pltpu.VMEM((depth - 1, quarter, width_all), bf16),
            pltpu.SemaphoreType.DMA((total_sends,)),
            pltpu.SemaphoreType.DMA((total_sends,)),
            pltpu.SemaphoreType.DMA((3,)),
        ],
        compiler_params=pltpu.CompilerParams(
            collective_id=0, has_side_effects=True, vmem_limit_bytes=60 * 1024 * 1024
        ),
    )(
        residual,
        queries,
        key_pairs,
        values,
        lambdas,
        head_gain[None],
        out_weight,
        mixer_gain[None],
        before_gain[None],
        after_gain[None],
        gate_weight,
        up_weight,
        down_in,
    )


def fits(mesh):
    return mesh.shape["tp"] == 4 and mesh.shape["sp"] == 8


def solution(mesh):
    return jax.shard_map(
        one_kernel if fits(mesh) else on_device,
        mesh=mesh,
        in_specs=(
            P(("sp", "tp"), None),
            P("sp", "tp"),
            P("sp", "tp"),
            P("sp", "tp"),
            P("tp"),
            P(),
            P(),
            P(),
            P(),
            P(),
            P("sp", "tp"),
            P("sp", "tp"),
            P("tp", "sp"),
        ),
        out_specs=P(("sp", "tp"), None),
        check_vma=False,
    )
```
